128 devices in a mesh: sp: 32 (over z, y, core), tp: 4 (over x).
Axes of the slice: x: 4, y: 4, z: 4, core: 2. Of those that a mesh axis runs over, the one named last changes fastest.
Arguments:
- tokens: bfloat16 [6, 8192, 2048], P(None, 'sp', 'tp'), may hold values from -6 to 6
- norm_gains: float32 [3, 2048], replicated, may hold values from 0.5 to 1.5
- weight_outer: bfloat16 [3, 2048, 1024], P(None, 'sp', 'tp'), may hold values from -0.125 to 0.125
- weight_inner: bfloat16 [3, 2048, 1024], P(None, 'sp', 'tp'), may hold values from -0.125 to 0.125
- weight_value: bfloat16 [3, 2048, 1024], P(None, 'sp', 'tp'), may hold values from -0.125 to 0.125
- conv_taps: bfloat16 [3, 3, 1024], P(None, None, 'tp'), may hold values from -3.5 to 3.5
- weight_output: bfloat16 [3, 1024, 2048], P(None, 'sp', 'tp'), may hold values from -0.1875 to 0.1875
Outputs:
- mixed_out: float32 [6, 8192, 2048], P(None, 'sp', 'tp')
The draws below stay inside these ranges and needn't reach their ends.
All inputs are finite; a program needn't handle non-finite values.
Results may differ from the reference program's by a relative error of at most 0.03.
Values may be sent and summed in bfloat16 or wider, within the bound.
No kernel may reach another device: no remote copies, remote signals or barrier semaphores. Data moves between devices by JAX's collectives and lax.ppermute only.
A program may use at most 128 MiB of HBM per device.

```python
import jax
import jax.numpy as jnp
from jax import lax

D = 2048
SC = 1024
KERNEL = 3
LAYERS = 3
SEQS = 6
SEQ = 8192


def shard_levels(key, dims, cuts, smallest, top_value):
    factor_of, own = 1.0, jax.random.fold_in(key, 6)
    for position, shards_of in cuts:
        draws = jnp.exp(jax.random.uniform(jax.random.fold_in(own, position), (shards_of,), jnp.float32, smallest / len(cuts), top_value / len(cuts)))
        factor_of = factor_of * jnp.repeat(draws, dims[position] // shards_of).reshape([-1 if axis == position else 1 for axis in range(len(dims))])
    return factor_of


def centred(stream_key, shape, scale, bound, pieces=(), held_as=jnp.bfloat16):
    values = scale * jax.random.normal(stream_key, shape, jnp.float32)
    if pieces:
        values = values * shard_levels(stream_key, shape, pieces, -0.22, 0.18)
    return jnp.clip(values, -bound, bound).astype(held_as)


def setup_inputs(seed: int = 0) -> dict:
    arg_keys = jax.random.split(jax.random.key(seed), 8)
    return {
        "tokens": centred(arg_keys[0], (SEQS, SEQ, D), 1.0, 6.0, ((1, 32), (2, 4))),
        "norm_gains": jnp.clip(1.0 + 0.1 * jax.random.normal(arg_keys[1], (LAYERS, D), jnp.float32), 0.5, 1.5),
        "weight_outer": centred(arg_keys[2], (LAYERS, D, SC), D ** -0.5, 0.125, ((1, 32), (2, 4))),
        "weight_inner": centred(arg_keys[3], (LAYERS, D, SC), D ** -0.5, 0.125, ((1, 32), (2, 4))),
        "weight_value": centred(arg_keys[4], (LAYERS, D, SC), D ** -0.5, 0.125, ((1, 32), (2, 4))),
        "conv_taps": centred(arg_keys[5], (LAYERS, KERNEL, SC), KERNEL ** -0.5, 3.5, ((2, 4),)),
        "weight_output": centred(arg_keys[6], (LAYERS, SC, D), SC ** -0.5, 0.1875, ((1, 32), (2, 4))),
    }


epsilon = 1e-06

def normalize(values_in, gain_row):
    values = values_in.astype(jnp.float32)
    scale = lax.rsqrt(lax.optimization_barrier(jnp.mean(values * values, axis=-1, keepdims=True)) + epsilon)
    return (values * scale * gain_row.astype(jnp.float32)).astype(jnp.bfloat16)

def reference(tokens, norm_gains, weight_outer, weight_inner, weight_value, conv_taps, weight_output):
    current = tokens
    projected = None
    for layer in range(LAYERS):
        normed = normalize(current, norm_gains[layer]).reshape(SEQS * SEQ, D)
        outer = jnp.dot(normed, weight_outer[layer], preferred_element_type=jnp.float32).astype(jnp.bfloat16)
        inner = jnp.dot(normed, weight_inner[layer], preferred_element_type=jnp.float32).astype(jnp.bfloat16)
        value = jnp.dot(normed, weight_value[layer], preferred_element_type=jnp.float32).astype(jnp.bfloat16)
        outer, inner, value = lax.optimization_barrier((outer, inner, value))
        gated = (inner.astype(jnp.float32) * value.astype(jnp.float32)).reshape(SEQS, SEQ, SC)
        padded = jnp.pad(gated, ((0, 0), (KERNEL - 1, 0), (0, 0)))
        conved = jnp.zeros((SEQS, SEQ, SC), jnp.float32)
        for offset in range(KERNEL):
            conved = conved + conv_taps[layer, offset].astype(jnp.float32) * padded[:, offset:offset + SEQ]
        mixer = (outer.astype(jnp.float32).reshape(SEQS, SEQ, SC) * conved).astype(jnp.bfloat16)
        projected = jnp.dot(mixer.reshape(SEQS * SEQ, SC), weight_output[layer], preferred_element_type=jnp.float32)
        current = projected.astype(jnp.bfloat16).reshape(SEQS, SEQ, D)
    return projected.reshape(SEQS, SEQ, D)
```

```python
import jax
import jax.numpy as jnp
from jax import lax
from jax.experimental import pallas as pl
from jax.experimental.pallas import tpu as pltpu
from jax.sharding import PartitionSpec as P

epsilon = 1e-06

SEQS, D, SC, LAYERS, KERNEL = 6, 2048, 1024, 3, 3
SP, TP = 32, 4
HALO = 8
OWN = 64
SPAN = OWN + HALO
ROWS = SEQS * SPAN
KIN, KOUT = D // SP, SC // SP
CB = SC // TP
FB = D // TP
PACK = LAYERS * 4 * KIN
TAPROWS = 16


def layers_kernel(x_ref, gains_ref, taps_ref, g_ref, out_ref, win, wout, cur, normed, mixer, sem_in, sem_out):
    def in_copies(layer, x):
        slot = layer % 2
        return [
            pltpu.make_async_copy(
                g_ref.at[:, x, pl.ds((layer * 4 + m) * KIN, KIN), :],
                win.at[slot, m, :, :, pl.ds(x * CB, CB)],
                sem_in.at[slot, x, m],
            )
            for m in range(3)
        ]

    def out_copies(layer, x):
        slot = layer % 2
        return [
            pltpu.make_async_copy(
                g_ref.at[:, x, pl.ds((layer * 4 + 3) * KIN + h * KOUT, KOUT), :],
                wout.at[slot, :, :, pl.ds(x * FB + h * CB, CB)],
                sem_out.at[slot, x, h],
            )
            for h in range(2)
        ]

    def start_in(layer):
        for x in range(TP):
            for c in in_copies(layer, x):
                c.start()

    def start_out(layer):
        for x in range(TP):
            for c in out_copies(layer, x):
                c.start()

    start_in(0)
    start_out(0)
    start_in(1)
    start_out(1)
    for x in range(TP):
        cur[:, x * FB : (x + 1) * FB] = x_ref[x]

    for layer in range(LAYERS):
        slot = layer % 2

        @pl.loop(0, ROWS // 16)
        def _(r):
            rows = pl.ds(pl.multiple_of(r * 16, 16), 16)
            v = cur[rows, :].astype(jnp.float32)
            scale = lax.rsqrt(jnp.sum(v * v, axis=-1, keepdims=True) * (1.0 / D) + epsilon)
            normed[rows, :] = (v * scale * gains_ref[layer : layer + 1, :]).astype(jnp.bfloat16)

        for x in range(TP):
            for c in in_copies(layer, x):
                c.wait()
            parts = []
            for m in range(3):
                w = win[slot, m, :, :, x * CB : (x + 1) * CB].reshape(D, CB)
                parts.append(
                    jnp.dot(normed[...], w, preferred_element_type=jnp.float32)
                    .astype(jnp.bfloat16)
                    .astype(jnp.float32)
                )
            outer, inner, value = parts
            gated = inner * value
            taps = taps_ref[x, layer * KERNEL : (layer + 1) * KERNEL, :].astype(jnp.float32)
            conved = taps[0:1] * pltpu.roll(gated, 2, 0)
            conved = conved + taps[1:2] * pltpu.roll(gated, 1, 0)
            conved = conved + taps[2:3] * gated
            mixer[:, x * CB : (x + 1) * CB] = (outer * conved).astype(jnp.bfloat16)
        if layer + 2 < LAYERS:
            start_in(layer + 2)

        for x in range(TP):
            for c in out_copies(layer, x):
                c.wait()
            w = wout[slot, :, :, x * FB : (x + 1) * FB].reshape(SC, FB)
            y = jnp.dot(mixer[...], w, preferred_element_type=jnp.float32)
            if layer + 1 < LAYERS:
                cur[:, x * FB : (x + 1) * FB] = y.astype(jnp.bfloat16)
            else:
                out_ref[x] = y.reshape(SEQS, SPAN, FB)[:, HALO:, :].astype(jnp.bfloat16)
        if layer + 2 < LAYERS:
            start_out(layer + 2)


def run_layers(x, gains, taps, g):
    flops = LAYERS * 2 * ROWS * SC * D * 4
    return pl.pallas_call(
        layers_kernel,
        out_shape=jax.ShapeDtypeStruct((TP, SEQS, OWN, FB), jnp.bfloat16),
        in_specs=[pl.BlockSpec(memory_space=pltpu.VMEM)] * 3 + [pl.BlockSpec(memory_space=pl.ANY)],
        out_specs=pl.BlockSpec(memory_space=pltpu.VMEM),
        scratch_shapes=[
            pltpu.VMEM((2, 3, SP, KIN, SC), jnp.bfloat16),
            pltpu.VMEM((2, SP, KOUT, D), jnp.bfloat16),
            pltpu.VMEM((ROWS, D), jnp.bfloat16),
            pltpu.VMEM((ROWS, D), jnp.bfloat16),
            pltpu.VMEM((ROWS, SC), jnp.bfloat16),
            pltpu.SemaphoreType.DMA((2, TP, 3)),
            pltpu.SemaphoreType.DMA((2, TP, 2)),
        ],
        compiler_params=pltpu.CompilerParams(vmem_limit_bytes=60 * 1024 * 1024),
        cost_estimate=pl.CostEstimate(flops=flops, bytes_accessed=48 * 1024 * 1024, transcendentals=0),
        name="mixer_layers",
    )(x, gains, taps, g)


def body(tokens, norm_gains, weight_outer, weight_inner, weight_value, conv_taps, weight_output):
    halves = jnp.stack([weight_output[:, :, :CB], weight_output[:, :, CB:]], axis=1).reshape(LAYERS, 1, KIN, CB)
    packed = jnp.concatenate(
        [jnp.stack([weight_outer, weight_inner, weight_value], axis=1), halves], axis=1
    ).reshape(PACK, CB)
    taps = jnp.pad(conv_taps.reshape(LAYERS * KERNEL, CB), ((0, TAPROWS - LAYERS * KERNEL), (0, 0)))
    packed = jnp.concatenate([packed, taps], axis=0)
    g = lax.all_gather(packed, ("sp", "tp")).reshape(SP, TP, PACK + TAPROWS, CB)

    before = lax.ppermute(tokens[:, -HALO:], "sp", [(i, i + 1) for i in range(SP - 1)])
    extended = jnp.concatenate([before, tokens], axis=1)
    send = jnp.stack([extended[:, i * OWN : i * OWN + SPAN] for i in range(TP)])
    x = lax.all_to_all(send, "tp", split_axis=0, concat_axis=0).reshape(TP, ROWS, FB)

    out = run_layers(x, norm_gains, g[0, :, PACK:, :], g)
    back = lax.all_to_all(out, "tp", split_axis=0, concat_axis=0)
    return jnp.moveaxis(back, 0, 1).reshape(SEQS, TP * OWN, FB).astype(jnp.float32)


def solution(mesh):
    in_specs = (
        P(None, "sp", "tp"),
        P(),
        P(None, "sp", "tp"),
        P(None, "sp", "tp"),
        P(None, "sp", "tp"),
        P(None, None, "tp"),
        P(None, "sp", "tp"),
    )
    return jax.shard_map(body, mesh=mesh, in_specs=in_specs, out_specs=P(None, "sp", "tp"), check_vma=False)
```

```python
import jax
import jax.numpy as jnp
from jax import lax
from jax.experimental import pallas as pl
from jax.experimental.pallas import tpu as pltpu
from jax.sharding import PartitionSpec as P

epsilon = 1e-06

SEQS, D, SC, LAYERS, KERNEL = 6, 2048, 1024, 3, 3
SP, TP = 32, 4
HALO = 8
OWN = 64
SPAN = OWN + HALO
ROWS = SEQS * SPAN
KIN, KOUT = D // SP, SC // SP
CB = SC // TP
FB = D // TP
PACK = LAYERS * 4 * KIN
TAPROWS = 16


def layers_kernel(x_ref, gains_ref, taps_ref, g_ref, out_ref, win, wout, xg, mixer, sem_in, sem_out):
    def in_copies(layer, x):
        slot = layer % 2
        return [
            pltpu.make_async_copy(
                g_ref.at[:, x, pl.ds((layer * 4 + m) * KIN, KIN), :],
                win.at[slot, m, :, :, pl.ds(x * CB, CB)],
                sem_in.at[slot, x, m],
            )
            for m in range(3)
        ]

    def out_copies(layer, x):
        slot = layer % 2
        return [
            pltpu.make_async_copy(
                g_ref.at[:, x, pl.ds((layer * 4 + 3) * KIN + h * KOUT, KOUT), :],
                wout.at[slot, :, :, pl.ds(x * FB + h * CB, CB)],
                sem_out.at[slot, x, h],
            )
            for h in range(2)
        ]

    def start_in(layer):
        for x in range(TP):
            for c in in_copies(layer, x):
                c.start()

    def start_out(layer):
        for x in range(TP):
            for c in out_copies(layer, x):
                c.start()

    start_in(0)
    start_out(0)
    start_in(1)
    start_out(1)
    sumsq = jnp.zeros((ROWS, 128), jnp.float32)
    for x in range(TP):
        v = x_ref[x].astype(jnp.float32)
        xg[:, x * FB : (x + 1) * FB] = (v * gains_ref[0:1, x * FB : (x + 1) * FB]).astype(jnp.bfloat16)
        for i in range(FB // 128):
            part = v[:, i * 128 : (i + 1) * 128]
            sumsq = sumsq + part * part

    for layer in range(LAYERS):
        slot = layer % 2
        scale = lax.rsqrt(jnp.sum(sumsq, axis=-1, keepdims=True) * (1.0 / D) + epsilon)

        for x in range(TP):
            for c in in_copies(layer, x):
                c.wait()
            parts = []
            for m in range(3):
                w = win[slot, m, :, :, x * CB : (x + 1) * CB].reshape(D, CB)
                parts.append(jnp.dot(xg[...], w, preferred_element_type=jnp.float32) * scale)
            outer, inner, value = parts
            gated = inner * value
            taps = taps_ref[x, layer * KERNEL : (layer + 1) * KERNEL, :].astype(jnp.float32)
            conved = taps[0:1] * pltpu.roll(gated, 2, 0)
            conved = conved + taps[1:2] * pltpu.roll(gated, 1, 0)
            conved = conved + taps[2:3] * gated
            mixer[:, x * CB : (x + 1) * CB] = (outer * conved).astype(jnp.bfloat16)
        if layer + 2 < LAYERS:
            start_in(layer + 2)

        sumsq = jnp.zeros((ROWS, 128), jnp.float32)
        for x in range(TP):
            for c in out_copies(layer, x):
                c.wait()
            w = wout[slot, :, :, x * FB : (x + 1) * FB].reshape(SC, FB)
            y = jnp.dot(mixer[...], w, preferred_element_type=jnp.float32)
            if layer + 1 < LAYERS:
                gains = gains_ref[layer + 1 : layer + 2, x * FB : (x + 1) * FB]
                xg[:, x * FB : (x + 1) * FB] = (y * gains).astype(jnp.bfloat16)
                for i in range(FB // 128):
                    part = y[:, i * 128 : (i + 1) * 128]
                    sumsq = sumsq + part * part
            else:
                out_ref[x] = y.reshape(SEQS, SPAN, FB)[:, HALO:, :].astype(jnp.bfloat16)
        if layer + 2 < LAYERS:
            start_out(layer + 2)


def run_layers(x, gains, taps, g):
    flops = LAYERS * 2 * ROWS * SC * D * 4
    return pl.pallas_call(
        layers_kernel,
        out_shape=jax.ShapeDtypeStruct((TP, SEQS, OWN, FB), jnp.bfloat16),
        in_specs=[pl.BlockSpec(memory_space=pltpu.VMEM)] * 3 + [pl.BlockSpec(memory_space=pl.ANY)],
        out_specs=pl.BlockSpec(memory_space=pltpu.VMEM),
        scratch_shapes=[
            pltpu.VMEM((2, 3, SP, KIN, SC), jnp.bfloat16),
            pltpu.VMEM((2, SP, KOUT, D), jnp.bfloat16),
            pltpu.VMEM((ROWS, D), jnp.bfloat16),
            pltpu.VMEM((ROWS, SC), jnp.bfloat16),
            pltpu.SemaphoreType.DMA((2, TP, 3)),
            pltpu.SemaphoreType.DMA((2, TP, 2)),
        ],
        compiler_params=pltpu.CompilerParams(vmem_limit_bytes=60 * 1024 * 1024),
        cost_estimate=pl.CostEstimate(flops=flops, bytes_accessed=48 * 1024 * 1024, transcendentals=0),
        name="mixer_layers",
    )(x, gains, taps, g)


def body(tokens, norm_gains, weight_outer, weight_inner, weight_value, conv_taps, weight_output):
    halves = jnp.stack([weight_output[:, :, :CB], weight_output[:, :, CB:]], axis=1).reshape(LAYERS, 1, KIN, CB)
    packed = jnp.concatenate(
        [jnp.stack([weight_outer, weight_inner, weight_value], axis=1), halves], axis=1
    ).reshape(PACK, CB)
    taps = jnp.pad(conv_taps.reshape(LAYERS * KERNEL, CB), ((0, TAPROWS - LAYERS * KERNEL), (0, 0)))
    packed = jnp.concatenate([packed, taps], axis=0)
    g = lax.all_gather(packed, ("sp", "tp")).reshape(SP, TP, PACK + TAPROWS, CB)

    before = lax.ppermute(tokens[:, -HALO:], "sp", [(i, i + 1) for i in range(SP - 1)])
    extended = jnp.concatenate([before, tokens], axis=1)
    send = jnp.stack([extended[:, i * OWN : i * OWN + SPAN] for i in range(TP)])
    x = lax.all_to_all(send, "tp", split_axis=0, concat_axis=0).reshape(TP, ROWS, FB)

    out = run_layers(x, norm_gains, g[0, :, PACK:, :], g)
    back = lax.all_to_all(out, "tp", split_axis=0, concat_axis=0)
    return jnp.moveaxis(back, 0, 1).reshape(SEQS, TP * OWN, FB).astype(jnp.float32)


def solution(mesh):
    in_specs = (
        P(None, "sp", "tp"),
        P(),
        P(None, "sp", "tp"),
        P(None, "sp", "tp"),
        P(None, "sp", "tp"),
        P(None, None, "tp"),
        P(None, "sp", "tp"),
    )
    return jax.shard_map(body, mesh=mesh, in_specs=in_specs, out_specs=P(None, "sp", "tp"), check_vma=False)
```
